32 devices in a mesh: grp: 2 (over y), sp: 8 (over z, core), tp: 2 (over x).
Axes of the slice: x: 2, y: 2, z: 4, core: 2. Of those that a mesh axis runs over, the one named last changes fastest.
Arguments:
- residual_in: bfloat16 [5120, 2048], P(('grp', 'sp', 'tp')), parts along dimension 0, may hold values from -6 to 6
- narrow_query_rows: bfloat16 [5120, 1024], P(('grp', 'sp'), 'tp'), parts along dimension 0, may hold values from -5 to 5
- wide_query_rows: bfloat16 [5120, 1024], P(('grp', 'sp'), 'tp'), parts along dimension 0, may hold values from -5 to 5
- narrow_key_value: bfloat16 [5120, 4, 128], P(('grp', 'sp'), 'tp'), parts along dimension 0, may hold values from -120 to 120
- wide_key_value: bfloat16 [5120, 4, 256], P(('grp', 'sp'), 'tp'), parts along dimension 0, may hold values from -120 to 120
- narrow_norm_gains: float32 [2, 64], replicated, may hold values from 0.1 to 10
- wide_norm_gains: float32 [2, 128], replicated, may hold values from 0.1 to 10
- out_narrow: bfloat16 [1024, 2048], P('tp'), may hold values from -0.1875 to 0.1875
- out_wide: bfloat16 [1024, 2048], P('tp'), may hold values from -0.1875 to 0.1875
- mixer_gain: float32 [2048], replicated, may hold values from 0.1 to 1.9
- mixer_gate: bfloat16 [2048, 5632], P('sp', 'tp'), may hold values from -0.125 to 0.125
- mixer_up: bfloat16 [2048, 5632], P('sp', 'tp'), may hold values from -0.125 to 0.125
- mixer_down: bfloat16 [5632, 2048], P('tp', 'sp'), may hold values from -0.078125 to 0.078125
Outputs:
- layer_out: bfloat16 [5120, 2048], P(('grp', 'sp', 'tp')), parts along dimension 0
The draws below stay inside these ranges and needn't reach their ends.
There are 2 independent parts, one for each index of `grp`. The reference program is written for one: setup_inputs(seed, part) draws one part's arguments, and reference() takes and returns one part's arrays. A program takes and returns all parts, laid end to end along the dimension named above; an argument that names none is the same for every part. Nothing has to cross between parts.
All inputs are finite; a program needn't handle non-finite values.
Results may differ from the reference program's by a relative error of at most 0.015.
The reference program's roundings to bfloat16 on the way count: a program that leaves them out, or rounds other values in their place, can miss the bound.
Values may be sent and summed in bfloat16 or wider, within the bound.
A program may use at most 128 MiB of HBM per device.

```python
import math
import jax
import jax.numpy as jnp
from jax import lax

D = 2048
FF = 5632
NARROW_HEAD_SIZE = 64
WIDE_HEAD_SIZE = 128
NARROW_QUERIES = 16
NARROW_KEY_HEADS = 4
WIDE_QUERIES = 8
WIDE_KEY_HEADS = 4
GRID = 64
TOKENS = 2560
N_TP = 2


def plain_entries(key, shape):
    return jnp.clip(jax.random.normal(key, shape, jnp.float32), -5.0, 5.0)


def value_entries(key, shape):
    return jnp.clip(24.0 * jax.random.normal(key, shape, jnp.float32), -120.0, 120.0)


def group_keys(key, heads, width, salt):
    return plain_entries(jax.random.fold_in(key, salt), (TOKENS, heads, width))


def group_query_heads(key, heads, key_heads, width, salt):
    queries = plain_entries(jax.random.fold_in(key, salt + 1), (TOKENS, heads, width))
    return queries.reshape(TOKENS, heads * width)


def group_key_value(key, heads, width, salt):
    keys = group_keys(key, heads, width, salt)
    values = value_entries(jax.random.fold_in(key, salt + 2), (TOKENS, heads, width))
    return jnp.concatenate([keys, values], axis=-1)


def group_gains(key, width, salt):
    inner = jax.random.fold_in(key, salt)
    return jnp.clip(1.0 + 0.18 * jax.random.normal(inner, (2, width), jnp.float32), 0.1, 1.9)


def draw_narrow_query_rows(key, part):
    return group_query_heads(key, NARROW_QUERIES, NARROW_KEY_HEADS, NARROW_HEAD_SIZE, 100).astype(jnp.bfloat16)


def draw_wide_query_rows(key, part):
    return group_query_heads(key, WIDE_QUERIES, WIDE_KEY_HEADS, WIDE_HEAD_SIZE, 200).astype(jnp.bfloat16)


def draw_narrow_key_value(key, part):
    return group_key_value(key, NARROW_KEY_HEADS, NARROW_HEAD_SIZE, 100).astype(jnp.bfloat16)


def draw_wide_key_value(key, part):
    return group_key_value(key, WIDE_KEY_HEADS, WIDE_HEAD_SIZE, 200).astype(jnp.bfloat16)


def draw_narrow_norm_gains(key, part):
    return group_gains(key, NARROW_HEAD_SIZE, 300)


def draw_wide_norm_gains(key, part):
    return group_gains(key, WIDE_HEAD_SIZE, 400)


def level_of(stream_key, dims, split, low, top_value):
    def one(dim, blocks):
        heights = jax.random.uniform(jax.random.fold_in(jax.random.fold_in(stream_key, 6), dim), (blocks,), jnp.float32, low / len(split), top_value / len(split))
        return jnp.repeat(jnp.exp(heights), dims[dim] // blocks).reshape((-1,) + (1,) * (len(dims) - dim - 1))

    factor_of = one(*split[0])
    for cut in split[1:]:
        factor_of = factor_of * one(*cut)
    return factor_of


def scatter_about(key, extent, scale, bound, shards=(), kind=jnp.bfloat16):
    entries = scale * jax.random.normal(key, extent, jnp.float32)
    if shards:
        entries = entries * level_of(key, extent, shards, -0.22, 0.18)
    return jnp.clip(entries, -bound, bound).astype(kind)


def setup_inputs(seed: int = 0, part: int = 0) -> dict:
    key_list = jax.random.split(jax.random.key(seed), 14)
    own_keys = jax.random.split(jax.random.fold_in(key_list[13], part), 14)
    residual_in = scatter_about(own_keys[0], (TOKENS, D), 1.0, 6.0, ((0, 16),))
    narrow_query_rows = draw_narrow_query_rows(jax.random.fold_in(jax.random.fold_in(key_list[13], part), 71), part)
    wide_query_rows = draw_wide_query_rows(jax.random.fold_in(jax.random.fold_in(key_list[13], part), 71), part)
    narrow_key_value = draw_narrow_key_value(jax.random.fold_in(jax.random.fold_in(key_list[13], part), 71), part)
    wide_key_value = draw_wide_key_value(jax.random.fold_in(jax.random.fold_in(key_list[13], part), 71), part)
    narrow_norm_gains = draw_narrow_norm_gains(jax.random.fold_in(key_list[13], 71), part)
    wide_norm_gains = draw_wide_norm_gains(jax.random.fold_in(key_list[13], 71), part)
    out_narrow = scatter_about(key_list[7], (NARROW_QUERIES * NARROW_HEAD_SIZE, D), (NARROW_QUERIES * NARROW_HEAD_SIZE) ** -0.5, 0.1875, ((0, 2),))
    out_wide = scatter_about(key_list[8], (WIDE_QUERIES * WIDE_HEAD_SIZE, D), (WIDE_QUERIES * WIDE_HEAD_SIZE) ** -0.5, 0.1875, ((0, 2),))
    mixer_gain = jnp.clip(1.0 + 0.18 * jax.random.normal(key_list[9], (D,), jnp.float32), 0.1, 1.9)
    mixer_gate = scatter_about(key_list[10], (D, FF), D ** -0.5, 0.125, ((0, 8), (1, 2)))
    mixer_up = scatter_about(key_list[11], (D, FF), D ** -0.5, 0.125, ((0, 8), (1, 2)))
    mixer_down = scatter_about(key_list[12], (FF, D), FF ** -0.5, 0.078125, ((0, 2), (1, 8)))
    return {"residual_in": residual_in, "narrow_query_rows": narrow_query_rows, "wide_query_rows": wide_query_rows, "narrow_key_value": narrow_key_value, "wide_key_value": wide_key_value, "narrow_norm_gains": narrow_norm_gains, "wide_norm_gains": wide_norm_gains, "out_narrow": out_narrow, "out_wide": out_wide, "mixer_gain": mixer_gain, "mixer_gate": mixer_gate, "mixer_up": mixer_up, "mixer_down": mixer_down}


eps = 1e-06
theta = 10000.0

def rounded(value):
    return lax.optimization_barrier(value.astype(jnp.bfloat16)).astype(jnp.float32)

def grid_angles(width):
    positions = jnp.arange(TOKENS, dtype=jnp.int32)
    quarter = width // 4
    freqs = theta ** (-jnp.arange(quarter, dtype=jnp.float32) * 4.0 / width)
    row = (positions // GRID).astype(jnp.float32)
    column = (positions % GRID).astype(jnp.float32)
    return jnp.concatenate([row[:, None] * freqs[None, :], column[:, None] * freqs[None, :]], axis=-1)

def prepare(raw, gain, angles):
    field = raw.astype(jnp.float32)
    field = field * lax.rsqrt(lax.optimization_barrier(jnp.mean(field * field, axis=-1, keepdims=True)) + eps) * gain.astype(jnp.float32)
    half = field.shape[-1] // 2
    cosine = jnp.cos(angles)[:, None, :]
    sine = jnp.sin(angles)[:, None, :]
    first = field[..., :half]
    second = field[..., half:]
    turned = jnp.concatenate([first * cosine - second * sine, second * cosine + first * sine], axis=-1)
    return rounded(turned)

def attend_heads(query_raw, keyval, gains, heads, key_heads, width):
    angles = grid_angles(width)
    queries = prepare(query_raw.reshape(TOKENS, heads, width), gains[0], angles)
    keys = prepare(keyval[:, :, :width], gains[1], angles)
    values = keyval[:, :, width:].astype(jnp.float32)
    group = heads // key_heads
    block = math.gcd(TOKENS, 128)
    blocks = queries.reshape(TOKENS // block, block, key_heads, group, width)

    def one(piece):
        scores = jnp.einsum('qkgd,skd->kgqs', piece, keys) / math.sqrt(width)
        peak = lax.optimization_barrier(jnp.max(scores, axis=-1, keepdims=True))
        weights = jnp.exp(scores - peak)
        total = lax.optimization_barrier(jnp.sum(weights, axis=-1))
        summed = jnp.einsum('kgqs,skd->qkgd', rounded(weights), values)
        return (summed / jnp.transpose(total, (2, 0, 1))[..., None]).astype(jnp.bfloat16)
    result = lax.map(one, blocks)
    return result.reshape(TOKENS, heads * width)

def reference(residual_in, narrow_query_rows, wide_query_rows, narrow_key_value, wide_key_value, narrow_norm_gains, wide_norm_gains, out_narrow, out_wide, mixer_gain, mixer_gate, mixer_up, mixer_down):
    attention_narrow = attend_heads(narrow_query_rows, narrow_key_value, narrow_norm_gains, NARROW_QUERIES, NARROW_KEY_HEADS, NARROW_HEAD_SIZE)
    attention_wide = attend_heads(wide_query_rows, wide_key_value, wide_norm_gains, WIDE_QUERIES, WIDE_KEY_HEADS, WIDE_HEAD_SIZE)
    cols_narrow = NARROW_QUERIES * NARROW_HEAD_SIZE // N_TP
    cols_wide = WIDE_QUERIES * WIDE_HEAD_SIZE // N_TP
    attended = jnp.zeros((TOKENS, D), jnp.float32)
    for index in range(N_TP):
        lo_n = index * cols_narrow
        lo_w = index * cols_wide
        part = jnp.dot(attention_narrow[:, lo_n:lo_n + cols_narrow], out_narrow[lo_n:lo_n + cols_narrow], preferred_element_type=jnp.float32)
        part = part + jnp.dot(attention_wide[:, lo_w:lo_w + cols_wide], out_wide[lo_w:lo_w + cols_wide], preferred_element_type=jnp.float32)
        attended = attended + rounded(part)
    attended = attended.astype(jnp.bfloat16)
    stream = residual_in.astype(jnp.float32) + attended.astype(jnp.float32)
    scale = lax.rsqrt(lax.optimization_barrier(jnp.mean(stream * stream, axis=-1, keepdims=True)) + eps)
    normed = (stream * scale * mixer_gain.astype(jnp.float32)).astype(jnp.bfloat16)
    gate = jnp.dot(normed, mixer_gate, preferred_element_type=jnp.float32)
    up = jnp.dot(normed, mixer_up, preferred_element_type=jnp.float32)
    hidden = (jax.nn.silu(gate) * up).astype(jnp.bfloat16)
    units = FF // N_TP
    branch = jnp.zeros((TOKENS, D), jnp.float32)
    for index in range(N_TP):
        lo_u = index * units
        branch = branch + rounded(jnp.dot(hidden[:, lo_u:lo_u + units], mixer_down[lo_u:lo_u + units], preferred_element_type=jnp.float32))
    branch = branch.astype(jnp.bfloat16)
    return (stream + branch.astype(jnp.float32)).astype(jnp.bfloat16)
```

```python
import math

import jax
import jax.numpy as jnp
from jax import lax
from jax.sharding import PartitionSpec as P

GRID = 64


eps = 1e-06
theta = 10000.0


def grid_angles(positions, width):
    quarter = width // 4
    freqs = theta ** (-jnp.arange(quarter, dtype=jnp.float32) * 4.0 / width)
    row = (positions // GRID).astype(jnp.float32)
    column = (positions % GRID).astype(jnp.float32)
    return jnp.concatenate(
        [row[:, None] * freqs[None, :], column[:, None] * freqs[None, :]], axis=-1
    )


def prepare(raw, gain, angles):
    field = raw.astype(jnp.float32)
    field = field * lax.rsqrt(jnp.mean(field * field, axis=-1, keepdims=True) + eps) * gain
    half = field.shape[-1] // 2
    cosine = jnp.cos(angles)[:, None, :]
    sine = jnp.sin(angles)[:, None, :]
    first = field[..., :half]
    second = field[..., half:]
    turned = jnp.concatenate(
        [first * cosine - second * sine, second * cosine + first * sine], axis=-1
    )
    return turned.astype(jnp.bfloat16)


def arrange(raw, gain, angles, key_heads, width):
    tokens = raw.shape[0]
    heads = raw.shape[1] // width
    queries = prepare(raw.reshape(tokens, heads, width), gain, angles)
    queries = queries.reshape(tokens, key_heads, heads // key_heads, width)
    return jnp.transpose(queries, (1, 2, 0, 3)).reshape(
        key_heads, heads // key_heads * tokens, width
    )


def own_keys(keyval, gain, angles, width):
    keys = prepare(keyval[:, :, :width], gain, angles)
    return jnp.concatenate([keys, keyval[:, :, width:]], axis=-1)


def block_extent(length):
    for extent in range(min(length, 2048), 0, -1):
        if length % extent == 0:
            return extent
    return 1


def absorb(state, keyval, queries, width):
    maxima, totals, summed = state
    keys = keyval[:, :, :width]
    values = keyval[:, :, width:]
    scores = jnp.einsum(
        "krd,skd->krs", queries, keys, preferred_element_type=jnp.float32
    ) / math.sqrt(width)
    peak = jnp.maximum(maxima, jnp.max(scores, axis=-1))
    rescale = jnp.exp(maxima - peak)
    weights = jnp.exp(scores - peak[..., None])
    totals = totals * rescale + jnp.sum(weights, axis=-1)
    summed = summed * rescale[..., None] + jnp.einsum(
        "krs,skd->krd", weights.astype(jnp.bfloat16), values, preferred_element_type=jnp.float32
    )
    return (peak, totals, summed)


def sweep(state, piece, queries, width):
    length = piece.shape[0]
    extent = block_extent(length)
    blocks = piece.reshape(length // extent, extent, piece.shape[1], piece.shape[2])

    def visit(carry, keyval):
        return (absorb(carry, keyval, queries, width), None)

    state, unused = lax.scan(visit, state, blocks)
    return state


def start_state(queries):
    rows_here = queries.shape[1]
    heads_here = queries.shape[0]
    return (
        jnp.full((heads_here, rows_here), -jnp.inf, jnp.float32),
        jnp.zeros((heads_here, rows_here), jnp.float32),
        jnp.zeros((heads_here, rows_here, queries.shape[2]), jnp.float32),
    )


def finish(state, groups, tokens):
    maxima, totals, summed = state
    attn = (summed / totals[..., None]).astype(jnp.bfloat16)
    return attn.reshape(attn.shape[0], groups, tokens, attn.shape[2])


def own_share(weight, dim):
    extent = weight.shape[dim] // lax.axis_size("grp")
    return lax.dynamic_slice_in_dim(weight, lax.axis_index("grp") * extent, extent, dim)


def local(
    residual_in,
    narrow_query_rows,
    wide_query_rows,
    narrow_key_value,
    wide_key_value,
    narrow_norm_gains,
    wide_norm_gains,
    out_narrow,
    out_wide,
    mixer_gain,
    mixer_gate,
    mixer_up,
    mixer_down,
):
    tokens = narrow_query_rows.shape[0]
    narrow_width = narrow_key_value.shape[2] // 2
    wide_width = wide_key_value.shape[2] // 2
    narrow_heads = narrow_key_value.shape[1]
    wide_heads = wide_key_value.shape[1]
    positions = lax.axis_index("sp") * tokens + jnp.arange(tokens, dtype=jnp.int32)
    angles_narrow = grid_angles(positions, narrow_width)
    angles_wide = grid_angles(positions, wide_width)
    queries_narrow = arrange(
        narrow_query_rows, narrow_norm_gains[0], angles_narrow, narrow_heads, narrow_width
    )
    queries_wide = arrange(wide_query_rows, wide_norm_gains[0], angles_wide, wide_heads, wide_width)
    sent_narrow = own_keys(narrow_key_value, narrow_norm_gains[1], angles_narrow, narrow_width)
    sent_wide = own_keys(wide_key_value, wide_norm_gains[1], angles_wide, wide_width)
    sent = jnp.concatenate([sent_narrow, sent_wide], axis=-1)
    whole = lax.all_gather(sent, "sp", axis=0, tiled=True)
    whole, gate_share, up_share, down_share = lax.optimization_barrier(
        (
            whole,
            own_share(mixer_gate, 0),
            own_share(mixer_up, 0),
            own_share(mixer_down, 1),
        )
    )
    gate_whole = lax.all_gather(gate_share, ("sp", "grp"), axis=0, tiled=True)
    up_whole = lax.all_gather(up_share, ("sp", "grp"), axis=0, tiled=True)
    split = narrow_key_value.shape[2]
    pieces = (whole[:, :, :split], whole[:, :, split:])
    state_narrow = sweep(start_state(queries_narrow), pieces[0], queries_narrow, narrow_width)
    state_wide = sweep(start_state(queries_wide), pieces[1], queries_wide, wide_width)
    groups_narrow = queries_narrow.shape[1] // tokens
    groups_wide = queries_wide.shape[1] // tokens
    attention_narrow = finish(state_narrow, groups_narrow, tokens)
    attention_wide = finish(state_wide, groups_wide, tokens)
    attention_narrow, attention_wide, gate_whole, up_whole = lax.optimization_barrier(
        (attention_narrow, attention_wide, gate_whole, up_whole)
    )
    weight_narrow = out_narrow.reshape(
        narrow_heads, groups_narrow, narrow_width, out_narrow.shape[1]
    )
    weight_wide = out_wide.reshape(wide_heads, groups_wide, wide_width, out_wide.shape[1])
    total = jnp.einsum(
        "kgtd,kgdn->tn", attention_narrow, weight_narrow, preferred_element_type=jnp.float32
    )
    attended = lax.psum_scatter(
        (
            total
            + jnp.einsum(
                "kgtd,kgdn->tn", attention_wide, weight_wide, preferred_element_type=jnp.float32
            )
        ).astype(jnp.bfloat16),
        "tp",
        scatter_dimension=0,
        tiled=True,
    )
    stream = residual_in.astype(jnp.float32) + attended.astype(jnp.float32)
    scale = lax.rsqrt(jnp.mean(stream * stream, axis=-1, keepdims=True) + eps)
    normed = (stream * scale * mixer_gain).astype(jnp.bfloat16)
    whole_rows = lax.all_gather(normed, "tp", axis=0, tiled=True)
    gate = jnp.dot(whole_rows, gate_whole, preferred_element_type=jnp.float32)
    up = jnp.dot(whole_rows, up_whole, preferred_element_type=jnp.float32)
    hidden = (jax.nn.silu(gate) * up).astype(jnp.bfloat16)
    terms = jnp.dot(
        hidden,
        lax.all_gather(down_share, ("sp", "grp"), axis=1, tiled=True),
        preferred_element_type=jnp.float32,
    )
    branch = lax.psum_scatter(terms.astype(jnp.bfloat16), "tp", scatter_dimension=0, tiled=True)
    return (stream + branch.astype(jnp.float32)).astype(jnp.bfloat16)


def solution(mesh):
    placed = (
        P(("grp", "sp", "tp"), None),
        P(("grp", "sp"), "tp"),
        P(("grp", "sp"), "tp"),
        P(("grp", "sp"), "tp", None),
        P(("grp", "sp"), "tp", None),
        P(),
        P(),
        P("tp", None),
        P("tp", None),
        P(),
        P("sp", "tp"),
        P("sp", "tp"),
        P("tp", "sp"),
    )
    return jax.shard_map(
        local, mesh=mesh, in_specs=placed, out_specs=P(("grp", "sp", "tp"), None), check_vma=False
    )
```

```python
import functools
import math

import jax
import jax.numpy as jnp
from jax import lax
from jax.experimental import pallas as pl
from jax.experimental.pallas import tpu as pltpu
from jax.sharding import PartitionSpec as P

GRID = 64
CORES = 2


eps = 1e-06
theta = 10000.0


def grid_angles(positions, width):
    quarter = width // 4
    freqs = theta ** (-jnp.arange(quarter, dtype=jnp.float32) * 4.0 / width)
    row = (positions // GRID).astype(jnp.float32)
    column = (positions % GRID).astype(jnp.float32)
    return jnp.concatenate(
        [row[:, None] * freqs[None, :], column[:, None] * freqs[None, :]], axis=-1
    )


def prepare(raw, gain, angles):
    field = raw.astype(jnp.float32)
    field = field * lax.rsqrt(jnp.mean(field * field, axis=-1, keepdims=True) + eps) * gain
    half = field.shape[-1] // 2
    cosine = jnp.cos(angles)[:, None, :]
    sine = jnp.sin(angles)[:, None, :]
    first = field[..., :half]
    second = field[..., half:]
    turned = jnp.concatenate(
        [first * cosine - second * sine, second * cosine + first * sine], axis=-1
    )
    return turned.astype(jnp.bfloat16)


def arrange(raw, gain, angles, key_heads, width):
    tokens = raw.shape[0]
    heads = raw.shape[1] // width
    queries = prepare(raw.reshape(tokens, heads, width), gain, angles)
    queries = queries.reshape(tokens, key_heads, heads // key_heads, width)
    return jnp.transpose(queries, (1, 2, 0, 3)).reshape(
        key_heads, heads // key_heads * tokens, width
    )


def own_keys(keyval, gain, angles, width):
    keys = prepare(keyval[:, :, :width], gain, angles)
    return jnp.concatenate([keys, keyval[:, :, width:]], axis=-1)


def block_extent(length):
    for extent in range(min(length, 2048), 0, -1):
        if length % extent == 0:
            return extent
    return 1


def absorb(state, keyval, queries, width):
    maxima, totals, summed = state
    keys = keyval[:, :, :width]
    values = keyval[:, :, width:]
    scores = jnp.einsum(
        "krd,skd->krs", queries, keys, preferred_element_type=jnp.float32
    ) / math.sqrt(width)
    peak = jnp.maximum(maxima, jnp.max(scores, axis=-1))
    rescale = jnp.exp(maxima - peak)
    weights = jnp.exp(scores - peak[..., None])
    totals = totals * rescale + jnp.sum(weights, axis=-1)
    summed = summed * rescale[..., None] + jnp.einsum(
        "krs,skd->krd", weights.astype(jnp.bfloat16), values, preferred_element_type=jnp.float32
    )
    return (peak, totals, summed)


def sweep(state, piece, queries, width):
    length = piece.shape[0]
    extent = block_extent(length)
    blocks = piece.reshape(length // extent, extent, piece.shape[1], piece.shape[2])

    def visit(carry, keyval):
        return (absorb(carry, keyval, queries, width), None)

    state, unused = lax.scan(visit, state, blocks)
    return state


def start_state(queries):
    rows_here = queries.shape[1]
    heads_here = queries.shape[0]
    return (
        jnp.full((heads_here, rows_here), -jnp.inf, jnp.float32),
        jnp.zeros((heads_here, rows_here), jnp.float32),
        jnp.zeros((heads_here, rows_here, queries.shape[2]), jnp.float32),
    )


def finish(state, groups, tokens):
    maxima, totals, summed = state
    attn = (summed / totals[..., None]).astype(jnp.bfloat16)
    return attn.reshape(attn.shape[0], groups, tokens, attn.shape[2])


def own_share(weight, dim):
    extent = weight.shape[dim] // lax.axis_size("grp")
    return lax.dynamic_slice_in_dim(weight, lax.axis_index("grp") * extent, extent, dim)


def ring_kernel(lines, span, *refs):
    shares = refs[0:2]
    outs = refs[2:4]
    own, ring_send, ring_recv, peer_send, peer_recv, own_in, own_out = refs[4:]
    n = lines * span
    line = lax.axis_index("grp")
    at = lax.axis_index("sp")
    core = at % CORES
    column = at // CORES
    here = column * (1 - line) + (n - 1 - column) * line

    def place(spot):
        row = spot // span
        return row, spot * (1 - row) + (n - 1 - spot) * row

    def device(spot):
        row, col = place(spot)
        return {"grp": row, "sp": col * CORES + core}

    ahead = device((here + 1) % n)
    behind = device((here + n - 1) % n)
    peer = {"sp": column * CORES + 1 - core}
    targets = (ahead, behind)
    extent = shares[0].shape[0] // lines
    half = extent // 2

    barrier = pltpu.get_barrier_semaphore()
    for other in (ahead, behind, peer):
        pl.semaphore_signal(barrier, inc=1, device_id=other, device_id_type=pl.DeviceIdType.MESH)
    pl.semaphore_wait(barrier, 3)

    def rows(spot, way):
        row, col = place(spot)
        start = ((col * CORES + core) * lines + row) * extent + way * half
        return pl.ds(pl.multiple_of(start, half), half)

    def source(step, way, w):
        if step == 0:
            return shares[w].at[pl.ds(pl.multiple_of(line * extent + way * half, half), half)]
        return outs[w].at[rows(origin(step, way), way)]

    def origin(step, way):
        return (here + n - step) % n if way == 0 else (here + step) % n

    def hop(step, way, w):
        return pltpu.make_async_remote_copy(
            src_ref=source(step, way, w),
            dst_ref=outs[w].at[rows(origin(step, way), way)],
            send_sem=ring_send.at[way, step, w],
            recv_sem=ring_recv.at[way, step, w],
            device_id=targets[way],
            device_id_type=pl.DeviceIdType.MESH,
        )

    def across(step, way, w):
        return pltpu.make_async_remote_copy(
            src_ref=source(step, way, w),
            dst_ref=outs[w].at[rows(origin(step, way), way)],
            send_sem=peer_send.at[w],
            recv_sem=peer_recv.at[w],
            device_id=peer,
            device_id_type=pl.DeviceIdType.MESH,
        )

    def load(w):
        block = pl.ds(pl.multiple_of(line * extent, extent), extent)
        return pltpu.make_async_copy(shares[w].at[block], own.at[w], own_in.at[w])

    def store(w):
        start = (at * lines + line) * extent
        block = pl.ds(pl.multiple_of(start, extent), extent)
        return pltpu.make_async_copy(own.at[w], outs[w].at[block], own_out.at[w])

    sides = [(way, w) for w in range(2) for way in range(2)]
    for step in range(n):
        for way, w in sides:
            if step > 0:
                hop(step - 1, way, w).wait_recv()
            if step < n - 1:
                hop(step, way, w).start()
            across(step, way, w).start()
        if step == 0:
            for w in range(2):
                load(w).start()
            for w in range(2):
                load(w).wait()
                store(w).start()
    for w in range(2):
        store(w).wait()
    for step in range(n - 1):
        for way, w in sides:
            hop(step, way, w).wait_send()
    for w in range(2):
        total = outs[w].at[pl.ds(0, n * extent)]
        pltpu.make_async_copy(total, total, peer_send.at[w]).wait()
        pltpu.make_async_copy(total, total, peer_recv.at[w]).wait()


def gather_rows(gate, up):
    lines = lax.axis_size("grp")
    parts = lax.axis_size("sp")
    span = parts // CORES
    n = lines * span
    depth, width = gate.shape
    whole = jax.ShapeDtypeStruct((depth * parts, width), gate.dtype)
    return pl.pallas_call(
        functools.partial(ring_kernel, lines, span),
        out_shape=(whole, whole),
        in_specs=[pl.BlockSpec(memory_space=pl.ANY)] * 2,
        out_specs=(pl.BlockSpec(memory_space=pl.ANY),) * 2,
        scratch_shapes=[
            pltpu.VMEM((2, depth // lines, width), gate.dtype),
            pltpu.SemaphoreType.DMA((2, n - 1, 2)),
            pltpu.SemaphoreType.DMA((2, n - 1, 2)),
            pltpu.SemaphoreType.DMA((2,)),
            pltpu.SemaphoreType.DMA((2,)),
            pltpu.SemaphoreType.DMA((2,)),
            pltpu.SemaphoreType.DMA((2,)),
        ],
        compiler_params=pltpu.CompilerParams(collective_id=0, has_side_effects=True),
        cost_estimate=pl.CostEstimate(
            flops=100_000_000_000, bytes_accessed=4 * depth * parts * width, transcendentals=0
        ),
    )(gate, up)


def local(
    residual_in,
    narrow_query_rows,
    wide_query_rows,
    narrow_key_value,
    wide_key_value,
    narrow_norm_gains,
    wide_norm_gains,
    out_narrow,
    out_wide,
    mixer_gain,
    mixer_gate,
    mixer_up,
    mixer_down,
):
    tokens = narrow_query_rows.shape[0]
    narrow_width = narrow_key_value.shape[2] // 2
    wide_width = wide_key_value.shape[2] // 2
    narrow_heads = narrow_key_value.shape[1]
    wide_heads = wide_key_value.shape[1]
    positions = lax.axis_index("sp") * tokens + jnp.arange(tokens, dtype=jnp.int32)
    angles_narrow = grid_angles(positions, narrow_width)
    angles_wide = grid_angles(positions, wide_width)
    queries_narrow = arrange(
        narrow_query_rows, narrow_norm_gains[0], angles_narrow, narrow_heads, narrow_width
    )
    queries_wide = arrange(wide_query_rows, wide_norm_gains[0], angles_wide, wide_heads, wide_width)
    sent_narrow = own_keys(narrow_key_value, narrow_norm_gains[1], angles_narrow, narrow_width)
    sent_wide = own_keys(wide_key_value, wide_norm_gains[1], angles_wide, wide_width)
    sent = jnp.concatenate([sent_narrow, sent_wide], axis=-1)
    sent, gate_share, up_share, down_share = lax.optimization_barrier(
        (sent, mixer_gate, mixer_up, own_share(mixer_down, 1))
    )
    whole = lax.all_gather(sent, "sp", axis=0, tiled=True)
    down_whole = lax.all_gather(down_share, ("sp", "grp"), axis=1, tiled=True)
    gate_whole, up_whole = gather_rows(gate_share, up_share)
    whole, gate_whole, up_whole = lax.optimization_barrier((whole, gate_whole, up_whole))
    split = narrow_key_value.shape[2]
    pieces = (whole[:, :, :split], whole[:, :, split:])
    state_narrow = sweep(start_state(queries_narrow), pieces[0], queries_narrow, narrow_width)
    state_wide = sweep(start_state(queries_wide), pieces[1], queries_wide, wide_width)
    groups_narrow = queries_narrow.shape[1] // tokens
    groups_wide = queries_wide.shape[1] // tokens
    attention_narrow = finish(state_narrow, groups_narrow, tokens)
    attention_wide = finish(state_wide, groups_wide, tokens)
    attention_narrow, attention_wide, down_whole = lax.optimization_barrier(
        (attention_narrow, attention_wide, down_whole)
    )
    weight_narrow = out_narrow.reshape(
        narrow_heads, groups_narrow, narrow_width, out_narrow.shape[1]
    )
    weight_wide = out_wide.reshape(wide_heads, groups_wide, wide_width, out_wide.shape[1])
    total = jnp.einsum(
        "kgtd,kgdn->tn", attention_narrow, weight_narrow, preferred_element_type=jnp.float32
    )
    attended = lax.psum_scatter(
        (
            total
            + jnp.einsum(
                "kgtd,kgdn->tn", attention_wide, weight_wide, preferred_element_type=jnp.float32
            )
        ).astype(jnp.bfloat16),
        "tp",
        scatter_dimension=0,
        tiled=True,
    )
    stream = residual_in.astype(jnp.float32) + attended.astype(jnp.float32)
    scale = lax.rsqrt(jnp.mean(stream * stream, axis=-1, keepdims=True) + eps)
    normed = (stream * scale * mixer_gain).astype(jnp.bfloat16)
    whole_rows = lax.all_gather(normed, "tp", axis=0, tiled=True)
    gate = jnp.dot(whole_rows, gate_whole, preferred_element_type=jnp.float32)
    up = jnp.dot(whole_rows, up_whole, preferred_element_type=jnp.float32)
    hidden = (jax.nn.silu(gate) * up).astype(jnp.bfloat16)
    terms = jnp.dot(
        hidden,
        down_whole,
        preferred_element_type=jnp.float32,
    )
    branch = lax.psum_scatter(terms.astype(jnp.bfloat16), "tp", scatter_dimension=0, tiled=True)
    return (stream + branch.astype(jnp.float32)).astype(jnp.bfloat16)


def solution(mesh):
    placed = (
        P(("grp", "sp", "tp"), None),
        P(("grp", "sp"), "tp"),
        P(("grp", "sp"), "tp"),
        P(("grp", "sp"), "tp", None),
        P(("grp", "sp"), "tp", None),
        P(),
        P(),
        P("tp", None),
        P("tp", None),
        P(),
        P("sp", "tp"),
        P("sp", "tp"),
        P("tp", "sp"),
    )
    return jax.shard_map(
        local, mesh=mesh, in_specs=placed, out_specs=P(("grp", "sp", "tp"), None), check_vma=False
    )
```
